32 devices in a mesh: row: 16 (over z, y, x), col: 2 (over core).
Axes of the slice: x: 2, y: 2, z: 4, core: 2. Of those that a mesh axis runs over, the one named last changes fastest.
Arguments:
- tokens: bfloat16 [2, 6144, 2048], P('col', 'row'), may hold values from -6 to 6
- norm_gain: bfloat16 [2048], replicated, may hold values from 0.099609375 to 1.8984375
- in_weight: bfloat16 [2048, 512], P('row', 'col'), may hold values from -0.125 to 0.125
- out_weight: bfloat16 [512, 2048], P('col', 'row'), may hold values from -0.25 to 0.25
Outputs:
- mixed: bfloat16 [2, 6144, 2048], P('col', 'row')
The draws below stay inside these ranges and needn't reach their ends.
All inputs are finite; a program needn't handle non-finite values.
Results may differ from the reference program's by a relative error of at most 0.013.
Values may be sent and summed in bfloat16 or wider, within the bound.
A program may use at most 64 MiB of HBM per device.

```python
import jax
import jax.numpy as jnp
from jax import lax

D = 2048
FW = 512
GS = 64
GROUPS = 8
LEN = 6144
BATCH = 2


def block_scale(stream_key, extent, pieces, smallest, largest):
    def one(dim, parts):
        steps = jax.random.uniform(jax.random.fold_in(jax.random.fold_in(stream_key, 6), dim), (parts,), jnp.float32, smallest / len(pieces), largest / len(pieces))
        return jnp.repeat(jnp.exp(steps), extent[dim] // parts).reshape((-1,) + (1,) * (len(extent) - dim - 1))

    level = one(*pieces[0])
    for cut in pieces[1:]:
        level = level * one(*cut)
    return level


def bell_draw(key, extent, spread, limit, cuts=(), dtype=jnp.bfloat16):
    loudness = block_scale(key, extent, cuts, -0.22, 0.18) if cuts else 1.0
    values = jax.random.normal(key, extent, jnp.float32) * spread * loudness
    return jnp.minimum(jnp.maximum(values, -limit), limit).astype(dtype)


def setup_inputs(seed: int = 0) -> dict:
    streams_of = jax.random.split(jax.random.key(seed), 5)
    tokens = bell_draw(streams_of[0], (BATCH, LEN, D), 1.0, 6.0, ((0, 2), (1, 16)))
    norm_gain = jnp.clip(1.0 + 0.18 * jax.random.normal(streams_of[1], (D,), jnp.float32), 0.099609375, 1.8984375).astype(jnp.bfloat16)
    in_weight = bell_draw(streams_of[2], (D, FW), D ** -0.5, 0.125, ((0, 16), (1, 2)))
    out_weight = bell_draw(streams_of[3], (FW, D), FW ** -0.5, 0.25, ((0, 2), (1, 16)))
    return {"tokens": tokens, "norm_gain": norm_gain, "in_weight": in_weight, "out_weight": out_weight}


EPS = 1e-06

def mix_sequence(sequence, norm_gain, in_weight, out_weight):
    widened = sequence.astype(jnp.float32)
    inverse_rms = lax.rsqrt(lax.optimization_barrier(jnp.mean(widened * widened, axis=-1, keepdims=True)) + EPS)
    normed = (widened * inverse_rms * norm_gain.astype(jnp.float32)).astype(jnp.bfloat16)
    projected = jnp.dot(normed, in_weight, preferred_element_type=jnp.float32).astype(jnp.bfloat16)
    grouped = projected.astype(jnp.float32).reshape(LEN, GROUPS, GS)
    spectrum = jnp.fft.fftn(grouped, axes=(0, 2), norm='ortho')
    mixed_real = jnp.real(spectrum).reshape(LEN, FW).astype(jnp.bfloat16)
    return jnp.dot(mixed_real, out_weight, preferred_element_type=jnp.float32).astype(jnp.bfloat16)

def reference(tokens, norm_gain, in_weight, out_weight):
    return lax.map(lambda sequence: mix_sequence(sequence, norm_gain, in_weight, out_weight), tokens)
```

```python
import functools
import math

import jax
import jax.numpy as jnp
import numpy as np
from jax import lax
from jax.experimental import pallas as pl
from jax.experimental.pallas import tpu as pltpu
from jax.sharding import PartitionSpec as P

GS = 64
EPS = 1e-06
LANES = 128
F32 = jnp.float32
BF16 = jnp.bfloat16


def angles(left, right, modulus):
    product = np.arange(left)[:, None] * np.arange(right)[None, :] % modulus
    radians = product * (2.0 * math.pi / modulus)
    return np.cos(radians), np.sin(radians)


def channel_tables(narrow):
    cos, sin = angles(GS, GS, GS)
    half = narrow // 2
    forward = np.zeros((GS, GS))
    combine = np.zeros((GS, GS))
    for slot in range(GS):
        owner, place = divmod(slot, narrow)
        j = owner * half + place % half
        if place >= half and j > 0:
            forward[slot] = sin[j]
            combine[slot, j] = -1.0
            combine[slot, GS - j] = 1.0
        else:
            j = GS // 2 if place >= half else j
            forward[slot] = cos[j]
            combine[slot, j] = 1.0
            combine[slot, (GS - j) % GS] = 1.0
    copies = np.eye(LANES // GS)
    return np.kron(copies, forward), np.kron(copies, combine)


def tables(peers, rows, channels):
    narrow = channels // peers
    step = rows // peers
    length = peers * rows
    forward, combine = channel_tables(narrow)
    cos, sin = angles(peers, peers, peers)
    eye = np.eye(narrow)
    chunk = LANES // narrow
    first = np.concatenate(
        [
            np.kron(part[t : t + chunk], eye)
            for t in range(0, peers, chunk)
            for part in (cos, -sin)
        ]
    )
    turn = np.stack(angles(peers, rows, length)) / math.sqrt(length * GS)
    second = np.concatenate(angles(rows, rows, rows), axis=1)
    order = np.zeros((rows, rows))
    for t in range(peers):
        for u in range(step):
            order[u * peers + t, t * step + u] = 1.0
    return (
        jnp.asarray(forward, BF16),
        jnp.asarray(combine, BF16),
        jnp.asarray(first, BF16),
        jnp.asarray(turn, F32),
        jnp.asarray(second, BF16),
        jnp.asarray(order, BF16),
    )


def dot(a, b):
    return jnp.dot(a, b, preferred_element_type=F32)


def dot_nt(a, b):
    return lax.dot_general(a, b, (((1,), (1,)), ((), ())), preferred_element_type=F32)


def kernel(
    peers,
    cols,
    tokens_hbm,
    gain_ref,
    in_ref,
    out_w_ref,
    forward_ref,
    combine_ref,
    first_hbm,
    turn_hbm,
    second_hbm,
    order_hbm,
    result_ref,
    tokens,
    first,
    turn,
    second,
    order,
    normed,
    projected,
    w_in,
    w_out,
    send_one,
    got_one,
    lines,
    send_two,
    got_two,
    arranged,
    local_sem,
    g_send,
    g_recv,
    c_send,
    c_recv,
    x_send,
    x_recv,
):
    me = lax.axis_index("row")
    core = lax.axis_index("col")
    rows, width = tokens.shape
    channels = projected.shape[1]
    narrow = channels // peers
    half = narrow // 2
    step = rows // peers

    loads = [
        pltpu.make_async_copy(src, dst, local_sem.at[i])
        for i, (src, dst) in enumerate(
            (
                (tokens_hbm, tokens),
                (first_hbm, first),
                (turn_hbm, turn),
                (second_hbm, second),
                (order_hbm, order),
            )
        )
    ]
    for load in loads:
        load.start()

    def peer(o):
        return lax.rem(me + o, peers)

    def mate(o):
        return lax.rem(core + o, cols)

    barrier = pltpu.get_barrier_semaphore()
    for o in range(1, peers):
        pl.semaphore_signal(barrier, inc=1, device_id={"row": peer(o)})
    for o in range(1, cols):
        pl.semaphore_signal(barrier, inc=1, device_id={"col": mate(o)})
    pl.semaphore_wait(barrier, peers - 1 + cols - 1)

    def spread(which, src, buffer):
        copies = []
        for o in range(1, peers):
            copy = pltpu.make_async_remote_copy(
                src_ref=src,
                dst_ref=buffer.at[core, me],
                send_sem=g_send.at[which, o],
                recv_sem=g_recv.at[which, o],
                device_id={"row": peer(o)},
            )
            copy.start()
            copies.append(copy)
        own = pltpu.make_async_copy(src, buffer.at[core, me], g_send.at[which, 0])
        own.start()
        return copies, own

    def relay(which, buffer, copies, own):
        for copy in copies:
            copy.wait_recv()
        own.wait()
        passed = []
        for o in range(1, cols):
            copy = pltpu.make_async_remote_copy(
                src_ref=buffer.at[core],
                dst_ref=buffer.at[core],
                send_sem=c_send.at[which, o],
                recv_sem=c_recv.at[which, o],
                device_id={"col": mate(o)},
            )
            copy.start()
            passed.append(copy)
        return passed

    in_copies, in_own = spread(0, in_ref, w_in)

    loads[0].wait()
    gain = gain_ref[...].astype(F32)
    tile = 32

    def norm(i, carry):
        at = pl.ds(pl.multiple_of(i * tile, tile), tile)
        block = tokens[at, :].astype(F32)
        inverse = lax.rsqrt(jnp.mean(block * block, axis=-1, keepdims=True) + EPS)
        normed[at, :] = (block * inverse * gain).astype(BF16)
        return carry

    lax.fori_loop(0, rows // tile, norm, 0)

    in_passed = relay(0, w_in, in_copies, in_own)
    out_copies, out_own = spread(1, out_w_ref, w_out)
    for copy in in_passed:
        copy.wait_recv()

    part = channels // cols
    for c in range(cols):
        projected[:, c * part : (c + 1) * part] = dot(
            normed[...], w_in[c].reshape(width, part)
        ).astype(BF16)

    for b in range(0, channels, LANES):
        slots = dot_nt(forward_ref[...], projected[:, b : b + LANES]).astype(BF16)
        send_one[b // narrow : (b + LANES) // narrow] = slots.reshape(
            LANES // narrow, narrow, rows
        )

    def exchange(which, src, dst):
        copies = []
        for o in range(1, peers):
            copy = pltpu.make_async_remote_copy(
                src_ref=src.at[peer(o)],
                dst_ref=dst.at[me],
                send_sem=x_send.at[which, o],
                recv_sem=x_recv.at[which, o],
                device_id={"row": peer(o)},
            )
            copy.start()
            copies.append(copy)
        own = pltpu.make_async_copy(src.at[me], dst.at[me], x_send.at[which, 0])
        own.start()
        for copy in copies:
            copy.wait_recv()
        own.wait()
        return copies

    one_copies = exchange(0, send_one, got_one)
    for load in loads[1:]:
        load.wait()
    columns = got_one[...].reshape(channels, rows)
    place = lax.broadcasted_iota(jnp.int32, (narrow, rows), 0)
    leads = lax.rem(me * narrow, GS) == 0
    first_sine = jnp.where(leads, half + 1, half)
    sine = place >= first_sine
    chunk = LANES // narrow
    for t0 in range(0, peers, chunk):
        both = dot(first[2 * t0 * narrow : 2 * (t0 + chunk) * narrow, :], columns)
        for i in range(chunk):
            t = t0 + i
            real = both[i * narrow : (i + 1) * narrow]
            imag = both[LANES + i * narrow : LANES + (i + 1) * narrow]
            cos = turn[0, t : t + 1, :]
            sin = turn[1, t : t + 1, :]
            z_real = real * cos + imag * sin
            z_imag = imag * cos - real * sin
            at = slice(t * narrow, (t + 1) * narrow)
            lines[at, :rows] = jnp.where(sine, -z_imag, z_real)
            lines[at, rows:] = jnp.where(sine, z_real, z_imag)
    whole = dot_nt(second[...], lines[...].astype(BF16))
    send_two[...] = whole.reshape(peers, step, channels).astype(BF16)
    two_copies = exchange(1, send_two, got_two)

    out_passed = relay(1, w_out, out_copies, out_own)

    block_of = lax.broadcasted_iota(jnp.int32, (step, LANES), 1) // narrow
    for d0 in range(0, peers, chunk):
        for t0 in range(0, peers, chunk):
            held = [
                got_two[d0 + i, :, t0 * narrow : (t0 + chunk) * narrow].astype(F32)
                for i in range(chunk)
            ]
            for j in range(chunk):
                made = None
                for i in range(chunk):
                    shift = (i - j) * narrow % LANES
                    moved = pltpu.roll(held[i], shift, 1) if shift else held[i]
                    made = moved if made is None else jnp.where(block_of == i, moved, made)
                t = t0 + j
                arranged[t * step : (t + 1) * step, d0 * narrow : (d0 + chunk) * narrow] = made
    natural = dot(order[...], arranged[...].astype(BF16)).astype(BF16)
    mixed = jnp.concatenate(
        [
            dot(natural[:, b : b + LANES], combine_ref[...]).astype(BF16)
            for b in range(0, channels, LANES)
        ],
        axis=1,
    )
    for copy in out_passed:
        copy.wait_recv()
    wide = w_out.shape[3]
    group = max(1, 256 // wide)
    for p in range(0, peers, group):
        weight = jnp.concatenate(
            [w_out[:, p + i].reshape(channels, wide) for i in range(group)], axis=1
        )
        result_ref[:, p * wide : (p + group) * wide] = dot(mixed, weight).astype(BF16)

    for copy in in_copies + in_passed + out_copies + out_passed + one_copies + two_copies:
        copy.wait_send()


def body(peers, cols, tokens, norm_gain, in_weight, out_weight):
    rows, width = tokens.shape[1:]
    in_rows, in_cols = in_weight.shape
    out_rows, out_cols = out_weight.shape
    channels = in_cols * cols
    narrow = channels // peers
    step = rows // peers
    forward, combine, first, turn, second, order = tables(peers, rows, channels)
    vmem = pl.BlockSpec(memory_space=pltpu.VMEM)
    hbm = pl.BlockSpec(memory_space=pl.ANY)
    result = pl.pallas_call(
        functools.partial(kernel, peers, cols),
        out_shape=jax.ShapeDtypeStruct((rows, width), BF16),
        in_specs=[hbm, vmem, vmem, vmem, vmem, vmem, hbm, hbm, hbm, hbm],
        out_specs=vmem,
        scratch_shapes=[
            pltpu.VMEM((rows, width), BF16),
            pltpu.VMEM(first.shape, BF16),
            pltpu.VMEM(turn.shape, F32),
            pltpu.VMEM(second.shape, BF16),
            pltpu.VMEM(order.shape, BF16),
            pltpu.VMEM((rows, width), BF16),
            pltpu.VMEM((rows, channels), BF16),
            pltpu.VMEM((cols, peers, in_rows, in_cols), BF16),
            pltpu.VMEM((cols, peers, out_rows, out_cols), BF16),
            pltpu.VMEM((peers, narrow, rows), BF16),
            pltpu.VMEM((peers, narrow, rows), BF16),
            pltpu.VMEM((channels, 2 * rows), F32),
            pltpu.VMEM((peers, step, channels), BF16),
            pltpu.VMEM((peers, step, channels), BF16),
            pltpu.VMEM((rows, channels), F32),
            pltpu.SemaphoreType.DMA((5,)),
            pltpu.SemaphoreType.DMA((2, peers)),
            pltpu.SemaphoreType.DMA((2, peers)),
            pltpu.SemaphoreType.DMA((2, cols)),
            pltpu.SemaphoreType.DMA((2, cols)),
            pltpu.SemaphoreType.DMA((2, peers)),
            pltpu.SemaphoreType.DMA((2, peers)),
        ],
        compiler_params=pltpu.CompilerParams(
            collective_id=0, has_side_effects=True, vmem_limit_bytes=60 * 1024 * 1024
        ),
    )(tokens[0], norm_gain[None], in_weight, out_weight, forward, combine, first, turn, second, order)
    return result[None]


def solution(mesh):
    in_specs = (P("col", "row", None), P(), P("row", "col"), P("col", "row"))
    out_specs = P("col", "row", None)
    step = functools.partial(body, mesh.shape["row"], mesh.shape["col"])
    return jax.shard_map(step, mesh=mesh, in_specs=in_specs, out_specs=out_specs, check_vma=False)
```

```python
import functools
import math

import jax
import jax.numpy as jnp
import numpy as np
from jax import lax
from jax.experimental import pallas as pl
from jax.experimental.pallas import tpu as pltpu
from jax.sharding import PartitionSpec as P

GS = 64
EPS = 1e-06
LANES = 128
F32 = jnp.float32
BF16 = jnp.bfloat16


def angles(left, right, modulus):
    product = np.arange(left)[:, None] * np.arange(right)[None, :] % modulus
    radians = product * (2.0 * math.pi / modulus)
    return np.cos(radians), np.sin(radians)


def channel_tables(narrow):
    cos, sin = angles(GS, GS, GS)
    half = narrow // 2
    forward = np.zeros((GS, GS))
    combine = np.zeros((GS, GS))
    for slot in range(GS):
        owner, place = divmod(slot, narrow)
        j = owner * half + place % half
        if place >= half and j > 0:
            forward[slot] = sin[j]
            combine[slot, j] = -1.0
            combine[slot, GS - j] = 1.0
        else:
            j = GS // 2 if place >= half else j
            forward[slot] = cos[j]
            combine[slot, j] = 1.0
            combine[slot, (GS - j) % GS] = 1.0
    copies = np.eye(LANES // GS)
    return np.kron(copies, forward), np.kron(copies, combine)


def tables(peers, rows, channels):
    narrow = channels // peers
    step = rows // peers
    length = peers * rows
    forward, combine = channel_tables(narrow)
    cos, sin = angles(peers, peers, peers)
    eye = np.eye(narrow)
    chunk = LANES // narrow
    first = np.concatenate(
        [
            np.kron(part[t : t + chunk], eye)
            for t in range(0, peers, chunk)
            for part in (cos, -sin)
        ]
    )
    turn = np.stack(angles(peers, rows, length)) / math.sqrt(length * GS)
    second = np.concatenate(angles(rows, rows, rows), axis=1)
    order = np.zeros((rows, rows))
    for t in range(peers):
        for u in range(step):
            order[u * peers + t, t * step + u] = 1.0
    return (
        jnp.asarray(forward, BF16),
        jnp.asarray(combine, BF16),
        jnp.asarray(first, BF16),
        jnp.asarray(turn, F32),
        jnp.asarray(second, BF16),
        jnp.asarray(order, BF16),
    )


def gather_orders(peers):
    short = []
    stride, rest = 1, peers
    while len(short) < 2 and rest % 2 == 0:
        short.append((stride, 2))
        stride, rest = stride * 2, rest // 2
    long = [(stride, rest)] if rest > 1 else []
    return [long + short, long + short[::-1]]


def dot(a, b):
    return jnp.dot(a, b, preferred_element_type=F32)


def dot_nt(a, b):
    return lax.dot_general(a, b, (((1,), (1,)), ((), ())), preferred_element_type=F32)


def kernel(
    peers,
    cols,
    tokens_hbm,
    gain_ref,
    in_ref,
    out_w_ref,
    forward_ref,
    combine_ref,
    first_hbm,
    turn_hbm,
    second_hbm,
    order_hbm,
    result_ref,
    tokens,
    first,
    turn,
    second,
    order,
    normed,
    projected,
    w_in,
    w_out,
    send_one,
    got_one,
    lines,
    send_two,
    got_two,
    arranged,
    local_sem,
    own_sem,
    g_send,
    g_recv,
    c_send,
    c_recv,
    x_send,
    x_recv,
):
    me = lax.axis_index("row")
    core = lax.axis_index("col")
    rows, width = tokens.shape
    channels = first.shape[1]
    parts = g_send.shape[1]
    orders = gather_orders(peers)
    stages = len(orders[0])
    narrow = channels // peers
    half = narrow // 2
    step = rows // peers

    loads = [
        pltpu.make_async_copy(src, dst, local_sem.at[i])
        for i, (src, dst) in enumerate(
            (
                (tokens_hbm, tokens),
                (first_hbm, first),
                (turn_hbm, turn),
                (second_hbm, second),
                (order_hbm, order),
            )
        )
    ]
    for load in loads:
        load.start()

    def peer(o):
        return lax.rem(me + o, peers)

    def mate(o):
        return lax.rem(core + o, cols)

    barrier = pltpu.get_barrier_semaphore()
    for o in range(1, peers):
        pl.semaphore_signal(barrier, inc=1, device_id={"row": peer(o)})
    for o in range(1, cols):
        pl.semaphore_signal(barrier, inc=1, device_id={"col": mate(o)})
    pl.semaphore_wait(barrier, peers - 1 + cols - 1)

    class Gather:
        def __init__(self, which, src, buffer):
            self.which, self.src, self.buffer = which, src, buffer
            self.height = src.shape[0] // parts
            self.held = [[None] for _ in range(parts)]
            self.open = [[] for _ in range(parts)]
            self.sent = []
            self.count = [0] * parts
            self.own = pltpu.make_async_copy(src, buffer.at[core, me], own_sem.at[which])
            self.own.start()

        def issue(self, part, stage):
            stride, size = orders[part % len(orders)][stage]
            at = pl.ds(part * self.height, self.height)
            place = lax.rem(lax.div(me, stride), size)
            arrived = []
            for o in range(1, size):
                to = me + (lax.rem(place + o, size) - place) * stride
                origin = (lax.rem(place + size - o, size) - place) * stride
                for held in self.held[part]:
                    block = me if held is None else held
                    copy = pltpu.make_async_remote_copy(
                        src_ref=self.src.at[at]
                        if held is None
                        else self.buffer.at[core, block, at],
                        dst_ref=self.buffer.at[core, block, at],
                        send_sem=g_send.at[self.which, part, self.count[part]],
                        recv_sem=g_recv.at[self.which, part, self.count[part]],
                        device_id={"row": to},
                    )
                    copy.start()
                    self.count[part] += 1
                    self.open[part].append(copy)
                    self.sent.append(copy)
                    arrived.append(block + origin)
            self.held[part] += arrived

        def wait(self, part):
            for copy in self.open[part]:
                copy.wait_recv()
            self.open[part] = []

        def advance(self, stage):
            for part in range(parts):
                self.wait(part)
                self.issue(part, stage)

        def relay(self):
            self.own.wait()
            self.passed = []
            for part in range(parts):
                self.wait(part)
                at = pl.ds(part * self.height, self.height)
                for o in range(1, cols):
                    copy = pltpu.make_async_remote_copy(
                        src_ref=self.buffer.at[core, :, at],
                        dst_ref=self.buffer.at[core, :, at],
                        send_sem=c_send.at[self.which, part, o],
                        recv_sem=c_recv.at[self.which, part, o],
                        device_id={"col": mate(o)},
                    )
                    copy.start()
                    self.passed.append(copy)

        def finish(self):
            for copy in self.passed:
                copy.wait_recv()

    gather_in = Gather(0, in_ref, w_in)
    gather_out = Gather(1, out_w_ref, w_out)
    gather_in.advance(0)

    loads[0].wait()
    gain = gain_ref[...].astype(F32).reshape(1, width)
    tile = 32

    def norm(i, carry):
        at = pl.ds(pl.multiple_of(i * tile, tile), tile)
        block = tokens[at, :].astype(F32)
        inverse = lax.rsqrt(jnp.mean(block * block, axis=-1, keepdims=True) + EPS)
        normed[at, :] = (block * inverse * gain).astype(BF16)
        return carry

    lax.fori_loop(0, rows // tile, norm, 0)

    for stage in range(1, stages):
        gather_in.advance(stage)
    gather_out.advance(0)
    gather_in.relay()

    part = channels // cols
    for i in range(cols):
        if i == 1:
            gather_in.finish()
        c = mate(i)
        projected[c] = dot(normed[...], w_in[c].reshape(width, part)).astype(BF16)

    natural_channels = jnp.concatenate([projected[c] for c in range(cols)], axis=1)
    for b in range(0, channels, LANES):
        slots = dot_nt(forward_ref[...], natural_channels[:, b : b + LANES]).astype(BF16)
        send_one[b // narrow : (b + LANES) // narrow] = slots.reshape(
            LANES // narrow, narrow, rows
        )

    def exchange(which, src, dst):
        copies = []
        for o in range(1, peers):
            copy = pltpu.make_async_remote_copy(
                src_ref=src.at[peer(o)],
                dst_ref=dst.at[me],
                send_sem=x_send.at[which, o],
                recv_sem=x_recv.at[which, o],
                device_id={"row": peer(o)},
            )
            copy.start()
            copies.append(copy)
        own = pltpu.make_async_copy(src.at[me], dst.at[me], x_send.at[which, 0])
        own.start()
        return copies, own

    def land(copies, own):
        for copy in copies:
            copy.wait_recv()
        own.wait()

    one_copies, one_own = exchange(0, send_one, got_one)
    if stages > 1:
        gather_out.advance(1)
    land(one_copies, one_own)
    for stage in range(2, stages):
        gather_out.advance(stage)
    for load in loads[1:]:
        load.wait()
    columns = got_one[...].reshape(channels, rows)
    place = lax.broadcasted_iota(jnp.int32, (narrow, rows), 0)
    leads = lax.rem(me * narrow, GS) == 0
    first_sine = jnp.where(leads, half + 1, half)
    sine = place >= first_sine
    chunk = LANES // narrow
    for t0 in range(0, peers, chunk):
        both = dot(first[2 * t0 * narrow : 2 * (t0 + chunk) * narrow, :], columns)
        for i in range(chunk):
            t = t0 + i
            real = both[i * narrow : (i + 1) * narrow]
            imag = both[LANES + i * narrow : LANES + (i + 1) * narrow]
            cos = turn[0, t : t + 1, :]
            sin = turn[1, t : t + 1, :]
            z_real = real * cos + imag * sin
            z_imag = imag * cos - real * sin
            at = slice(t * narrow, (t + 1) * narrow)
            lines[at, :rows] = jnp.where(sine, -z_imag, z_real)
            lines[at, rows:] = jnp.where(sine, z_real, z_imag)
    whole = dot_nt(second[...], lines[...].astype(BF16))
    send_two[...] = whole.reshape(peers, step, channels).astype(BF16)
    two_copies, two_own = exchange(1, send_two, got_two)
    gather_out.relay()
    land(two_copies, two_own)

    block_of = lax.broadcasted_iota(jnp.int32, (step, LANES), 1) // narrow
    for d0 in range(0, peers, chunk):
        for t0 in range(0, peers, chunk):
            held = [
                got_two[d0 + i, :, t0 * narrow : (t0 + chunk) * narrow].astype(F32)
                for i in range(chunk)
            ]
            for j in range(chunk):
                made = None
                for i in range(chunk):
                    shift = (i - j) * narrow % LANES
                    moved = pltpu.roll(held[i], shift, 1) if shift else held[i]
                    made = moved if made is None else jnp.where(block_of == i, moved, made)
                t = t0 + j
                arranged[t * step : (t + 1) * step, d0 * narrow : (d0 + chunk) * narrow] = made
    natural = dot(order[...], arranged[...].astype(BF16)).astype(BF16)
    mixed = jnp.concatenate(
        [
            dot(natural[:, b : b + LANES], combine_ref[...]).astype(BF16)
            for b in range(0, channels, LANES)
        ],
        axis=1,
    )
    gather_out.finish()
    wide = w_out.shape[3]
    group = max(1, 256 // wide)
    for p in range(0, peers, group):
        weight = jnp.concatenate(
            [w_out[:, p + i].reshape(channels, wide) for i in range(group)], axis=1
        )
        result_ref[:, p * wide : (p + group) * wide] = dot(mixed, weight).astype(BF16)

    for copy in (
        gather_in.sent
        + gather_in.passed
        + gather_out.sent
        + gather_out.passed
        + one_copies
        + two_copies
    ):
        copy.wait_send()


def body(peers, cols, tokens, norm_gain, in_weight, out_weight):
    rows, width = tokens.shape[1:]
    in_rows, in_cols = in_weight.shape
    out_rows, out_cols = out_weight.shape
    channels = in_cols * cols
    narrow = channels // peers
    step = rows // peers
    parts = max(1, min(4, in_rows // 16, out_rows // 16))
    forward, combine, first, turn, second, order = tables(peers, rows, channels)
    vmem = pl.BlockSpec(memory_space=pltpu.VMEM)
    hbm = pl.BlockSpec(memory_space=pl.ANY)
    result = pl.pallas_call(
        functools.partial(kernel, peers, cols),
        out_shape=jax.ShapeDtypeStruct((rows, width), BF16),
        in_specs=[hbm, vmem, vmem, vmem, vmem, vmem, hbm, hbm, hbm, hbm],
        out_specs=vmem,
        scratch_shapes=[
            pltpu.VMEM((rows, width), BF16),
            pltpu.VMEM(first.shape, BF16),
            pltpu.VMEM(turn.shape, F32),
            pltpu.VMEM(second.shape, BF16),
            pltpu.VMEM(order.shape, BF16),
            pltpu.VMEM((rows, width), BF16),
            pltpu.VMEM((cols, rows, in_cols), BF16),
            pltpu.VMEM((cols, peers, in_rows, in_cols), BF16),
            pltpu.VMEM((cols, peers, out_rows, out_cols), BF16),
            pltpu.VMEM((peers, narrow, rows), BF16),
            pltpu.VMEM((peers, narrow, rows), BF16),
            pltpu.VMEM((channels, 2 * rows), F32),
            pltpu.VMEM((peers, step, channels), BF16),
            pltpu.VMEM((peers, step, channels), BF16),
            pltpu.VMEM((rows, channels), F32),
            pltpu.SemaphoreType.DMA((5,)),
            pltpu.SemaphoreType.DMA((2,)),
            pltpu.SemaphoreType.DMA((2, parts, peers)),
            pltpu.SemaphoreType.DMA((2, parts, peers)),
            pltpu.SemaphoreType.DMA((2, parts, cols)),
            pltpu.SemaphoreType.DMA((2, parts, cols)),
            pltpu.SemaphoreType.DMA((2, peers)),
            pltpu.SemaphoreType.DMA((2, peers)),
        ],
        compiler_params=pltpu.CompilerParams(
            collective_id=0, has_side_effects=True, vmem_limit_bytes=60 * 1024 * 1024
        ),
    )(tokens[0], norm_gain, in_weight, out_weight, forward, combine, first, turn, second, order)
    return result[None]


def solution(mesh):
    in_specs = (P("col", "row", None), P(), P("row", "col"), P("col", "row"))
    out_specs = P("col", "row", None)
    step = functools.partial(body, mesh.shape["row"], mesh.shape["col"])
    return jax.shard_map(step, mesh=mesh, in_specs=in_specs, out_specs=out_specs, check_vma=False)
```

```python
import functools
import math

import jax
import jax.numpy as jnp
import numpy as np
from jax import lax
from jax.experimental import pallas as pl
from jax.experimental.pallas import tpu as pltpu
from jax.sharding import PartitionSpec as P

GS = 64
EPS = 1e-06
LANES = 128
F32 = jnp.float32
BF16 = jnp.bfloat16


def angles(left, right, modulus):
    product = np.arange(left)[:, None] * np.arange(right)[None, :] % modulus
    radians = product * (2.0 * math.pi / modulus)
    return np.cos(radians), np.sin(radians)


def channel_tables(narrow):
    cos, sin = angles(GS, GS, GS)
    half = narrow // 2
    forward = np.zeros((GS, GS))
    combine = np.zeros((GS, GS))
    for slot in range(GS):
        owner, place = divmod(slot, narrow)
        j = owner * half + place % half
        if place >= half and j > 0:
            forward[slot] = sin[j]
            combine[slot, j] = -1.0
            combine[slot, GS - j] = 1.0
        else:
            j = GS // 2 if place >= half else j
            forward[slot] = cos[j]
            combine[slot, j] = 1.0
            combine[slot, (GS - j) % GS] = 1.0
    copies = np.eye(LANES // GS)
    return np.kron(copies, forward), np.kron(copies, combine)


def tables(peers, rows, channels):
    narrow = channels // peers
    step = rows // peers
    length = peers * rows
    forward, combine = channel_tables(narrow)
    cos, sin = angles(peers, peers, peers)
    eye = np.eye(narrow)
    chunk = LANES // narrow
    first = np.concatenate(
        [
            np.kron(part[t : t + chunk], eye)
            for t in range(0, peers, chunk)
            for part in (cos, -sin)
        ]
    )
    turn = np.stack(angles(peers, rows, length)) / math.sqrt(length * GS)
    second = np.concatenate(angles(rows, rows, rows), axis=1)
    order = np.zeros((rows, rows))
    for t in range(peers):
        for u in range(step):
            order[u * peers + t, t * step + u] = 1.0
    return (
        jnp.asarray(forward, BF16),
        jnp.asarray(combine, BF16),
        jnp.asarray(first, BF16),
        jnp.asarray(turn, F32),
        jnp.asarray(second, BF16),
        jnp.asarray(order, BF16),
    )


def gather_orders(peers):
    short = []
    stride, rest = 1, peers
    while len(short) < 2 and rest % 2 == 0:
        short.append((stride, 2))
        stride, rest = stride * 2, rest // 2
    long = [(stride, rest)] if rest > 1 else []
    return [long + short, long + short[::-1]]


def dot(a, b):
    return jnp.dot(a, b, preferred_element_type=F32)


def dot_nt(a, b):
    return lax.dot_general(a, b, (((1,), (1,)), ((), ())), preferred_element_type=F32)


def kernel(
    peers,
    cols,
    tokens_hbm,
    gain_ref,
    in_ref,
    out_w_ref,
    forward_ref,
    combine_ref,
    first_hbm,
    turn_hbm,
    second_hbm,
    order_hbm,
    result_ref,
    result,
    tokens,
    first,
    turn,
    second,
    order,
    normed,
    projected,
    w_in,
    w_out,
    send_one,
    got_one,
    lines,
    send_two,
    got_two,
    arranged,
    local_sem,
    own_sem,
    store_sem,
    g_send,
    g_recv,
    c_send,
    c_recv,
    x_send,
    x_recv,
):
    me = lax.axis_index("row")
    core = lax.axis_index("col")
    rows, width = tokens.shape
    channels = first.shape[1]
    parts = g_send.shape[1]
    orders = gather_orders(peers)
    stages = len(orders[0])
    narrow = channels // peers
    half = narrow // 2
    step = rows // peers

    loads = [
        pltpu.make_async_copy(src, dst, local_sem.at[i])
        for i, (src, dst) in enumerate(
            (
                (tokens_hbm, tokens),
                (first_hbm, first),
                (turn_hbm, turn),
                (second_hbm, second),
                (order_hbm, order),
            )
        )
    ]
    for load in loads:
        load.start()

    def peer(o):
        return lax.rem(me + o, peers)

    def mate(o):
        return lax.rem(core + o, cols)

    barrier = pltpu.get_barrier_semaphore()
    for o in range(1, peers):
        pl.semaphore_signal(barrier, inc=1, device_id={"row": peer(o)})
    for o in range(1, cols):
        pl.semaphore_signal(barrier, inc=1, device_id={"col": mate(o)})
    pl.semaphore_wait(barrier, peers - 1 + cols - 1)

    class Gather:
        def __init__(self, which, src, buffer):
            self.which, self.src, self.buffer = which, src, buffer
            self.height = src.shape[0] // parts
            self.held = [[None] for _ in range(parts)]
            self.open = [[] for _ in range(parts)]
            self.sent = []
            self.count = [0] * parts
            self.own = pltpu.make_async_copy(src, buffer.at[core, me], own_sem.at[which])
            self.own.start()

        def issue(self, part, stage):
            stride, size = orders[part % len(orders)][stage]
            at = pl.ds(part * self.height, self.height)
            place = lax.rem(lax.div(me, stride), size)
            arrived = []
            for o in range(1, size):
                to = me + (lax.rem(place + o, size) - place) * stride
                origin = (lax.rem(place + size - o, size) - place) * stride
                for held in self.held[part]:
                    block = me if held is None else held
                    copy = pltpu.make_async_remote_copy(
                        src_ref=self.src.at[at]
                        if held is None
                        else self.buffer.at[core, block, at],
                        dst_ref=self.buffer.at[core, block, at],
                        send_sem=g_send.at[self.which, part, self.count[part]],
                        recv_sem=g_recv.at[self.which, part, self.count[part]],
                        device_id={"row": to},
                    )
                    copy.start()
                    self.count[part] += 1
                    self.open[part].append(copy)
                    self.sent.append(copy)
                    arrived.append(block + origin)
            self.held[part] += arrived

        def wait(self, part):
            for copy in self.open[part]:
                copy.wait_recv()
            self.open[part] = []

        def advance(self, stage):
            for part in range(parts):
                self.wait(part)
                self.issue(part, stage)

        def relay(self):
            self.own.wait()
            self.passed = []
            for part in range(parts):
                self.wait(part)
                at = pl.ds(part * self.height, self.height)
                for o in range(1, cols):
                    copy = pltpu.make_async_remote_copy(
                        src_ref=self.buffer.at[core, :, at],
                        dst_ref=self.buffer.at[core, :, at],
                        send_sem=c_send.at[self.which, part, o],
                        recv_sem=c_recv.at[self.which, part, o],
                        device_id={"col": mate(o)},
                    )
                    copy.start()
                    self.passed.append(copy)

        def finish(self):
            for copy in self.passed:
                copy.wait_recv()

    gather_in = Gather(0, in_ref, w_in)
    gather_out = Gather(1, out_w_ref, w_out)
    gather_in.advance(0)

    loads[0].wait()
    gain = gain_ref[...].astype(F32).reshape(1, width)
    tile = 32

    def norm(i, carry):
        at = pl.ds(pl.multiple_of(i * tile, tile), tile)
        block = tokens[at, :].astype(F32)
        inverse = lax.rsqrt(jnp.mean(block * block, axis=-1, keepdims=True) + EPS)
        normed[at, :] = (block * inverse * gain).astype(BF16)
        return carry

    tiles = rows // tile
    cuts = [tiles * i // stages for i in range(stages + 1)]
    for stage in range(stages):
        if stage:
            gather_in.advance(stage)
        lax.fori_loop(cuts[stage], cuts[stage + 1], norm, 0)
    gather_out.advance(0)
    gather_in.relay()

    part = channels // cols
    for i in range(cols):
        if i == 1:
            gather_in.finish()
        c = mate(i)
        projected[c] = dot(normed[...], w_in[c].reshape(width, part)).astype(BF16)

    natural_channels = jnp.concatenate([projected[c] for c in range(cols)], axis=1)
    for b in range(0, channels, LANES):
        slots = dot_nt(forward_ref[...], natural_channels[:, b : b + LANES]).astype(BF16)
        send_one[b // narrow : (b + LANES) // narrow] = slots.reshape(
            LANES // narrow, narrow, rows
        )

    def exchange(which, src, dst):
        copies = []
        for o in range(1, peers):
            copy = pltpu.make_async_remote_copy(
                src_ref=src.at[peer(o)],
                dst_ref=dst.at[me],
                send_sem=x_send.at[which, o],
                recv_sem=x_recv.at[which, o],
                device_id={"row": peer(o)},
            )
            copy.start()
            copies.append(copy)
        own = pltpu.make_async_copy(src.at[me], dst.at[me], x_send.at[which, 0])
        own.start()
        return copies, own

    def land(copies, own):
        for copy in copies:
            copy.wait_recv()
        own.wait()

    one_copies, one_own = exchange(0, send_one, got_one)
    if stages > 1:
        gather_out.advance(1)
    land(one_copies, one_own)
    for stage in range(2, stages):
        gather_out.advance(stage)
    for load in loads[1:]:
        load.wait()
    columns = got_one[...].reshape(channels, rows)
    place = lax.broadcasted_iota(jnp.int32, (narrow, rows), 0)
    leads = lax.rem(me * narrow, GS) == 0
    first_sine = jnp.where(leads, half + 1, half)
    sine = place >= first_sine
    chunk = LANES // narrow
    for t0 in range(0, peers, chunk):
        both = dot(first[2 * t0 * narrow : 2 * (t0 + chunk) * narrow, :], columns)
        for i in range(chunk):
            t = t0 + i
            real = both[i * narrow : (i + 1) * narrow]
            imag = both[LANES + i * narrow : LANES + (i + 1) * narrow]
            cos = turn[0, t : t + 1, :]
            sin = turn[1, t : t + 1, :]
            z_real = real * cos + imag * sin
            z_imag = imag * cos - real * sin
            at = slice(t * narrow, (t + 1) * narrow)
            lines[at, :rows] = jnp.where(sine, -z_imag, z_real)
            lines[at, rows:] = jnp.where(sine, z_real, z_imag)
    whole = dot_nt(second[...], lines[...].astype(BF16))
    send_two[...] = whole.reshape(peers, step, channels).astype(BF16)
    two_copies, two_own = exchange(1, send_two, got_two)
    gather_out.relay()
    land(two_copies, two_own)

    block_of = lax.broadcasted_iota(jnp.int32, (step, LANES), 1) // narrow
    for d0 in range(0, peers, chunk):
        for t0 in range(0, peers, chunk):
            held = [
                got_two[d0 + i, :, t0 * narrow : (t0 + chunk) * narrow].astype(F32)
                for i in range(chunk)
            ]
            for j in range(chunk):
                made = None
                for i in range(chunk):
                    shift = (i - j) * narrow % LANES
                    moved = pltpu.roll(held[i], shift, 1) if shift else held[i]
                    made = moved if made is None else jnp.where(block_of == i, moved, made)
                t = t0 + j
                arranged[t * step : (t + 1) * step, d0 * narrow : (d0 + chunk) * narrow] = made
    natural = dot(order[...], arranged[...].astype(BF16)).astype(BF16)
    mixed = jnp.concatenate(
        [
            dot(natural[:, b : b + LANES], combine_ref[...]).astype(BF16)
            for b in range(0, channels, LANES)
        ],
        axis=1,
    )
    gather_out.finish()
    stores = []
    wide = w_out.shape[3]
    group = max(1, 256 // wide)
    for p in range(0, peers, group):
        weight = jnp.concatenate(
            [w_out[:, p + i].reshape(channels, wide) for i in range(group)], axis=1
        )
        at = slice(p * wide, (p + group) * wide)
        result[:, at] = dot(mixed, weight).astype(BF16)
        store = pltpu.make_async_copy(result.at[:, at], result_ref.at[:, at], store_sem.at[p])
        store.start()
        stores.append(store)
    for store in stores:
        store.wait()

    for copy in (
        gather_in.sent
        + gather_in.passed
        + gather_out.sent
        + gather_out.passed
        + one_copies
        + two_copies
    ):
        copy.wait_send()


def body(peers, cols, tokens, norm_gain, in_weight, out_weight):
    rows, width = tokens.shape[1:]
    in_rows, in_cols = in_weight.shape
    out_rows, out_cols = out_weight.shape
    channels = in_cols * cols
    narrow = channels // peers
    step = rows // peers
    parts = max(1, min(4, in_rows // 16, out_rows // 16))
    forward, combine, first, turn, second, order = tables(peers, rows, channels)
    vmem = pl.BlockSpec(memory_space=pltpu.VMEM)
    hbm = pl.BlockSpec(memory_space=pl.ANY)
    result = pl.pallas_call(
        functools.partial(kernel, peers, cols),
        out_shape=jax.ShapeDtypeStruct((rows, width), BF16),
        in_specs=[hbm, vmem, vmem, vmem, vmem, vmem, hbm, hbm, hbm, hbm],
        out_specs=hbm,
        scratch_shapes=[
            pltpu.VMEM((rows, width), BF16),
            pltpu.VMEM((rows, width), BF16),
            pltpu.VMEM(first.shape, BF16),
            pltpu.VMEM(turn.shape, F32),
            pltpu.VMEM(second.shape, BF16),
            pltpu.VMEM(order.shape, BF16),
            pltpu.VMEM((rows, width), BF16),
            pltpu.VMEM((cols, rows, in_cols), BF16),
            pltpu.VMEM((cols, peers, in_rows, in_cols), BF16),
            pltpu.VMEM((cols, peers, out_rows, out_cols), BF16),
            pltpu.VMEM((peers, narrow, rows), BF16),
            pltpu.VMEM((peers, narrow, rows), BF16),
            pltpu.VMEM((channels, 2 * rows), F32),
            pltpu.VMEM((peers, step, channels), BF16),
            pltpu.VMEM((peers, step, channels), BF16),
            pltpu.VMEM((rows, channels), F32),
            pltpu.SemaphoreType.DMA((5,)),
            pltpu.SemaphoreType.DMA((2,)),
            pltpu.SemaphoreType.DMA((peers,)),
            pltpu.SemaphoreType.DMA((2, parts, peers)),
            pltpu.SemaphoreType.DMA((2, parts, peers)),
            pltpu.SemaphoreType.DMA((2, parts, cols)),
            pltpu.SemaphoreType.DMA((2, parts, cols)),
            pltpu.SemaphoreType.DMA((2, peers)),
            pltpu.SemaphoreType.DMA((2, peers)),
        ],
        compiler_params=pltpu.CompilerParams(
            collective_id=0, has_side_effects=True, vmem_limit_bytes=60 * 1024 * 1024
        ),
    )(tokens[0], norm_gain, in_weight, out_weight, forward, combine, first, turn, second, order)
    return result[None]


def solution(mesh):
    in_specs = (P("col", "row", None), P(), P("row", "col"), P("col", "row"))
    out_specs = P("col", "row", None)
    step = functools.partial(body, mesh.shape["row"], mesh.shape["col"])
    return jax.shard_map(step, mesh=mesh, in_specs=in_specs, out_specs=out_specs, check_vma=False)
```
